32 devices in a mesh: grp: 2 (over y), dp: 2 (over x), kv: 4 (over z), tp: 2 (over core).
Axes of the slice: x: 2, y: 2, z: 4, core: 2. Of those that a mesh axis runs over, the one named last changes fastest.
Arguments:
- candidate_vectors: bfloat16 [128, 4, 2048], P(('grp', 'dp'), None, ('kv', 'tp')), parts along dimension 0, may hold values from -6 to 6
- leading_scaling_factor: bfloat16 [2048], replicated, may hold values from 0.099609375 to 1.8984375
- lane_feed_matrix: bfloat16 [2048, 32, 2, 64], P(None, 'kv', 'tp')
- final_valve_matrix: bfloat16 [2048, 32, 2, 64], P(None, 'kv', 'tp'), may hold values from -0.125 to 0.125
- increment_matrix: bfloat16 [2048, 32, 2], replicated, may hold values from -0.125 to 0.125
- entry_basis_matrix: bfloat16 [2048, 2, 128], P(None, 'tp'), may hold values from -0.125 to 0.125
- readout_basis_matrix: bfloat16 [2048, 2, 128], P(None, 'tp'), may hold values from -0.125 to 0.125
- lane_feed_kernel: float32 [4, 32, 2, 64], P(None, 'kv', 'tp'), may hold values from -3 to 3
- entry_basis_kernel: float32 [4, 2, 128], P(None, 'tp'), may hold values from -3 to 3
- readout_basis_kernel: float32 [4, 2, 128], P(None, 'tp'), may hold values from -3 to 3
- increment_offset: float32 [32, 2], P('kv', 'tp'), may hold values from -4 to 1
- shrink_speed_exponent: float32 [32, 2], P('kv', 'tp'), may hold values from 0 to 2.8
- lane_bypass_factor: float32 [32, 2], P('kv', 'tp'), may hold values from 0.5 to 1.5
- final_linear_matrix: bfloat16 [32, 2, 64, 2048], P(None, None, None, ('kv', 'tp')), may hold values from -0.09375 to 0.09375
- hidden_carried_memory: float32 [128, 32, 2, 64, 128], P(('grp', 'dp'), 'kv', 'tp'), parts along dimension 0, may hold values from -0.6 to 0.6
- lane_filter_memory: bfloat16 [128, 7, 32, 2, 64], P(('grp', 'dp'), None, 'kv', 'tp'), parts along dimension 0, may hold values from -6 to 6
- entry_basis_memory: bfloat16 [128, 7, 2, 128], P(('grp', 'dp'), None, 'tp'), parts along dimension 0, may hold values from -6 to 6
- readout_basis_memory: bfloat16 [128, 7, 2, 128], P(('grp', 'dp'), None, 'tp'), parts along dimension 0, may hold values from -6 to 6
- predecessor_index: int32 [128, 4], P(('grp', 'dp')), parts along dimension 0, may hold values from -1 to 2, as said below
- admitted_counts: int32 [128], P(('grp', 'dp')), parts along dimension 0, may hold values from 0 to 4
- surplus_fading: float32 [128, 4, 32, 2], P(('grp', 'dp'), None, 'kv', 'tp'), parts along dimension 0, may hold values from -0.7 to 0, as said below
Outputs:
- mixed: bfloat16 [128, 4, 2048], P(('grp', 'dp'), None, ('kv', 'tp')), parts along dimension 0
The draws below stay inside these ranges and needn't reach their ends.
There are 2 independent parts, one for each index of `grp`. The reference program is written for one: setup_inputs(seed, part) draws one part's arguments, and reference() takes and returns one part's arrays. A program takes and returns all parts, laid end to end along the dimension named above; an argument that names none is the same for every part. Nothing has to cross between parts.
Inputs may be any that keep to these rules, and one draw needn't show every extreme that they name: predecessor_index[s, j] is -1 or a smaller proposal index than j. `surplus_fading`: zero except at a few proposals and heads.
All inputs are finite; a program needn't handle non-finite values.
Results may differ from the reference program's by a relative error of at most 0.012.
Values may be sent and summed in bfloat16 or wider, within the bound.
A program may use at most 64 MiB of HBM per device.

```python
import jax
import jax.numpy as jnp
from jax import lax

D = 2048
HG = 32
G = 2
HD = 64
N = 128
CONV = 4
PROP = 4
PREV = 4
WIN = 7
SEQS = 64


def draw_lane_feed_matrix(key, part):
    first, second = jax.random.split(key)
    base = jax.random.normal(first, (D, HG, G, HD), jnp.float32) * D ** (-0.5)
    order = (jnp.arange(HG)[:, None] * G + jnp.arange(G)[None, :]).astype(jnp.float32) / (HG * G - 1)
    spread = 3.0
    scale = spread ** (order - 0.5)
    jitter = jax.random.uniform(second, (HG, G, HD), jnp.float32, 0.7, 1.4)
    return (base * scale[None, :, :, None] * jitter[None]).astype(jnp.bfloat16)


def draw_predecessor_index(key, part):
    upper = jnp.arange(PROP, dtype=jnp.int32)[None, :]
    return jax.random.randint(key, (SEQS, PROP), -1, upper).astype(jnp.int32)


def draw_surplus_fading(key, part):
    first, second = jax.random.split(jax.random.fold_in(key, 7))
    struck = jax.random.uniform(first, (SEQS, PROP, HG, G), jnp.float32) < 0.15
    amount = jax.random.uniform(second, (SEQS, PROP, HG, G), jnp.float32, -0.7, -0.22)
    return jnp.where(struck, amount, 0.0)


def place_ends(array, key, low, top_value):
    longest = array.shape.index(max(array.shape))
    spots = []
    for shift in (0, 1):
        where = [jax.random.randint(jax.random.fold_in(key, axis), (), 0, length) for axis, length in enumerate(array.shape)]
        where[longest] = (where[longest] + shift) % array.shape[longest]
        spots.append(tuple(where))
    return array.at[spots[0]].set(low).at[spots[1]].set(top_value)


def steps_of(rng, extent, shards, smallest, largest):
    def one(dim, shards_of):
        steps = jax.random.uniform(jax.random.fold_in(jax.random.fold_in(rng, 6), dim), (shards_of,), jnp.float32, smallest / len(shards), largest / len(shards))
        return jnp.repeat(jnp.exp(steps), extent[dim] // shards_of).reshape((-1,) + (1,) * (len(extent) - dim - 1))

    factor_of = one(*shards[0])
    for cut in shards[1:]:
        factor_of = factor_of * one(*cut)
    return factor_of


def gaussian(stream_key, shape, scale, limit, cuts=(), kind=jnp.bfloat16):
    result = scale * jax.random.normal(stream_key, shape, jnp.float32)
    if cuts:
        result = result * steps_of(stream_key, shape, cuts, -0.22, 0.18)
    return jnp.clip(result, -limit, limit).astype(kind)


def setup_inputs(seed: int = 0, part: int = 0) -> dict:
    key_of = jax.random.split(jax.random.key(seed), 22)
    part_splits = jax.random.split(jax.random.fold_in(key_of[21], part), 22)
    return {
        "candidate_vectors": gaussian(part_splits[0], (SEQS, PROP, D), 1.0, 6.0, ((0, 2), (2, 8))),
        "leading_scaling_factor": jnp.clip(1.0 + 0.18 * jax.random.normal(key_of[1], (D,), jnp.float32), 0.099609375, 1.8984375).astype(jnp.bfloat16),
        "lane_feed_matrix": draw_lane_feed_matrix(jax.random.fold_in(key_of[21], 71), part),
        "final_valve_matrix": gaussian(key_of[3], (D, HG, G, HD), D ** -0.5, 0.125, ((1, 4), (2, 2))),
        "increment_matrix": gaussian(key_of[4], (D, HG, G), D ** -0.5, 0.125),
        "entry_basis_matrix": gaussian(key_of[5], (D, G, N), D ** -0.5, 0.125, ((1, 2),)),
        "readout_basis_matrix": gaussian(key_of[6], (D, G, N), D ** -0.5, 0.125, ((1, 2),)),
        "lane_feed_kernel": gaussian(key_of[7], (CONV, HG, G, HD), 0.5, 3.0, ((1, 4), (2, 2)), jnp.float32),
        "entry_basis_kernel": gaussian(key_of[8], (CONV, G, N), 0.5, 3.0, ((1, 2),), jnp.float32),
        "readout_basis_kernel": gaussian(key_of[9], (CONV, G, N), 0.5, 3.0, ((1, 2),), jnp.float32),
        "increment_offset": jnp.clip(-4.0 + 5.0 * jax.random.uniform(key_of[10], (HG, G), jnp.float32) ** steps_of(key_of[10], (HG, G), ((0, 4), (1, 2)), -0.2, 0.2), -4.0, 1.0),
        "shrink_speed_exponent": jnp.clip(2.8 * jax.random.uniform(key_of[11], (HG, G), jnp.float32) ** steps_of(key_of[11], (HG, G), ((0, 4), (1, 2)), -0.2, 0.2), 0.0, 2.8),
        "lane_bypass_factor": jnp.clip(0.5 + 1.0 * jax.random.uniform(key_of[12], (HG, G), jnp.float32) ** steps_of(key_of[12], (HG, G), ((0, 4), (1, 2)), -0.2, 0.2), 0.5, 1.5),
        "final_linear_matrix": gaussian(key_of[13], (HG, G, HD, D), (HG * G * HD) ** -0.5, 0.09375, ((3, 8),)),
        "hidden_carried_memory": gaussian(part_splits[14], (SEQS, HG, G, HD, N), 0.1, 0.6, ((0, 2), (1, 4), (2, 2)), jnp.float32),
        "lane_filter_memory": gaussian(part_splits[15], (SEQS, WIN, HG, G, HD), 1.0, 6.0, ((0, 2), (2, 4), (3, 2))),
        "entry_basis_memory": gaussian(part_splits[16], (SEQS, WIN, G, N), 1.0, 6.0, ((0, 2), (2, 2))),
        "readout_basis_memory": gaussian(part_splits[17], (SEQS, WIN, G, N), 1.0, 6.0, ((0, 2), (2, 2))),
        "predecessor_index": draw_predecessor_index(jax.random.fold_in(jax.random.fold_in(key_of[21], part), 71), part),
        "admitted_counts": place_ends(jax.random.randint(part_splits[19], (SEQS,), 0, PREV + 1), jax.random.fold_in(part_splits[19], 1), 0, PREV).astype(jnp.int32),
        "surplus_fading": draw_surplus_fading(jax.random.fold_in(jax.random.fold_in(key_of[21], part), 71), part),
    }


HIGH = lax.Precision.HIGHEST

def lineage_tables(predecessor_index):
    seqs, props = predecessor_index.shape
    column = jnp.arange(props, dtype=jnp.int32)
    current = jnp.broadcast_to(column[None, :], (seqs, props)).astype(jnp.int32)
    depth = jnp.zeros((seqs, props), jnp.int32)
    onehots = []
    for step in range(props):
        onehots.append((current[:, :, None] == column[None, None, :]).astype(jnp.float32))
        if step > 0:
            depth = depth + (current >= 0).astype(jnp.int32)
        upward = jnp.take_along_axis(predecessor_index, jnp.maximum(current, 0).astype(jnp.int32), axis=1)
        current = jnp.where(current >= 0, upward, -1).astype(jnp.int32)
    return (onehots, depth)

def conv_tree(current, saved, taps, onehots, depth, admitted_counts):
    props = current.shape[1]
    slots = jnp.arange(saved.shape[1], dtype=jnp.int32)
    cur_f = current.astype(jnp.float32)
    saved_f = saved.astype(jnp.float32)
    total = jnp.zeros(cur_f.shape, jnp.float32)
    for lag in range(CONV):
        value = jnp.zeros(cur_f.shape, jnp.float32)
        if lag < props:
            value = jnp.einsum('sji,sic->sjc', onehots[lag], cur_f, precision=HIGH)
        target = (admitted_counts[:, None] + (CONV - 1) - (lag - depth)).astype(jnp.int32)
        chosen = ((depth < lag)[:, :, None] & (slots[None, None, :] == target[:, :, None])).astype(jnp.float32)
        value = value + jnp.einsum('sjw,swc->sjc', chosen, saved_f, precision=HIGH)
        total = total + taps[CONV - 1 - lag].astype(jnp.float32) * value
    return jax.nn.silu(total)

def reference(candidate_vectors, leading_scaling_factor, lane_feed_matrix, final_valve_matrix, increment_matrix, entry_basis_matrix, readout_basis_matrix, lane_feed_kernel, entry_basis_kernel, readout_basis_kernel, increment_offset, shrink_speed_exponent, lane_bypass_factor, final_linear_matrix, hidden_carried_memory, lane_filter_memory, entry_basis_memory, readout_basis_memory, predecessor_index, admitted_counts, surplus_fading):
    seqs, props, _ = candidate_vectors.shape
    tok_f = candidate_vectors.astype(jnp.float32)
    r_in = lax.rsqrt(lax.optimization_barrier(jnp.mean(tok_f * tok_f, axis=-1)) + 1e-06).reshape(seqs * props, 1)
    scaled = (tok_f * leading_scaling_factor.astype(jnp.float32)).astype(jnp.bfloat16).reshape(seqs * props, D)

    def project(weight):
        return jnp.dot(scaled, weight.reshape(D, -1), preferred_element_type=jnp.float32) * r_in
    x_rows = project(lane_feed_matrix).astype(jnp.bfloat16).reshape(seqs, props, HG * G * HD)
    z_rows = project(final_valve_matrix).astype(jnp.bfloat16).reshape(seqs, props, HG, G, HD)
    dt_raw = project(increment_matrix).reshape(seqs, props, HG, G)
    b_rows = project(entry_basis_matrix).astype(jnp.bfloat16).reshape(seqs, props, G * N)
    c_rows = project(readout_basis_matrix).astype(jnp.bfloat16).reshape(seqs, props, G * N)
    onehots, depth = lineage_tables(predecessor_index)
    x_conv = conv_tree(x_rows, lane_filter_memory.reshape(seqs, WIN, -1), lane_feed_kernel.reshape(CONV, -1), onehots, depth, admitted_counts).reshape(seqs, props, HG, G, HD)
    b_conv = conv_tree(b_rows, entry_basis_memory.reshape(seqs, WIN, -1), entry_basis_kernel.reshape(CONV, -1), onehots, depth, admitted_counts).reshape(seqs, props, G, N)
    c_conv = conv_tree(c_rows, readout_basis_memory.reshape(seqs, WIN, -1), readout_basis_kernel.reshape(CONV, -1), onehots, depth, admitted_counts).reshape(seqs, props, G, N)
    lineage = sum(onehots)
    lane_increment = jax.nn.softplus(dt_raw + increment_offset)
    fading_exponent = -jnp.exp(shrink_speed_exponent) * lane_increment + surplus_fading
    level = jnp.einsum('sji,sihg->sjhg', lineage, fading_exponent, precision=HIGH)
    gap = level[:, :, None] - level[:, None, :]
    weight = jnp.where(lineage[:, :, :, None, None] > 0, jnp.exp(jnp.minimum(gap, 0.0)), 0.0)
    scores = jnp.einsum('sjgn,sign->sjig', c_conv, b_conv, precision=HIGH)
    mixing = weight * scores[:, :, :, None, :] * lane_increment[:, None]
    y_rows = jnp.einsum('sjihg,sihgp->sjhgp', mixing, x_conv, precision=HIGH)
    y_rows = y_rows + jnp.exp(level)[..., None] * jnp.einsum('shgpn,sjgn->sjhgp', hidden_carried_memory, c_conv, precision=HIGH)
    y_rows = y_rows + lane_bypass_factor[..., None] * x_conv
    gated = (y_rows * jax.nn.silu(z_rows.astype(jnp.float32))).astype(jnp.bfloat16).reshape(seqs * props, -1)
    gated_f = gated.astype(jnp.float32)
    r_out = lax.rsqrt(lax.optimization_barrier(jnp.mean(gated_f * gated_f, axis=-1)) + 1e-05)
    mixed = jnp.dot(gated, final_linear_matrix.reshape(-1, D), preferred_element_type=jnp.float32) * r_out[:, None]
    return mixed.astype(jnp.bfloat16).reshape(seqs, props, D)
```

```python
import functools

import jax
import jax.numpy as jnp
from jax import lax
from jax.experimental import pallas as pl
from jax.experimental.pallas import tpu as pltpu
from jax.sharding import PartitionSpec as P

CONV = 4
MESH = pl.DeviceIdType.MESH
HIGH = lax.Precision.HIGHEST
F32 = jnp.float32
BF16 = jnp.bfloat16
NT = (((1,), (1,)), ((), ()))


def silu(value):
    return value * jax.nn.sigmoid(value)


def mixer_kernel(
    n, seqs, props, heads, hd, chunks, d_model, heads_all,
    x_hbm, gain_ref, wx_hbm, wz_hbm, dtw_ref, wb_hbm, wc_hbm,
    xtap_ref, btap_ref, ctap_ref, offset_ref, shrink_ref, bypass_ref,
    fl_hbm, st_hbm, xsave_ref, bsave_ref, csave_ref, pred_ref, adm_ref, fade_ref,
    out_ref,
    xg, gg, wx, wz, wb, wc, fl, st, acc_x, acc_z, xrow, cs, ys,
    load_sem, st_sem, own_sem, s1, r1, s1b, r1b, s2, r2, s2b, r2b,
):
    kv = lax.axis_index("kv")
    tp = lax.axis_index("tp")
    other = 1 - tp
    rows = seqs * props
    feat = x_hbm.shape[1]
    wide = heads * hd
    cw = wide // chunks
    hpc = heads // chunks

    own = pltpu.make_async_copy(x_hbm, xg.at[0, tp], own_sem)
    own.start()
    barrier = pltpu.get_barrier_semaphore()
    for step in range(1, n):
        pl.semaphore_signal(
            barrier, inc=1, device_id={"kv": lax.rem(kv + step, n)}, device_id_type=MESH
        )
    pl.semaphore_signal(barrier, inc=1, device_id={"tp": other}, device_id_type=MESH)

    loads = []
    for index, (src, dst) in enumerate(
        ((wb_hbm, wb), (wc_hbm, wc), (wx_hbm, wx), (wz_hbm, wz), (fl_hbm, fl))
    ):
        loads.append(pltpu.make_async_copy(src, dst, load_sem.at[index]))
    parts = st_sem.shape[0]
    span = seqs // parts
    st_loads = [
        pltpu.make_async_copy(
            st_hbm.at[pl.ds(part * span, span)], st.at[pl.ds(part * span, span)], st_sem.at[part]
        )
        for part in range(parts)
    ]
    for copy in loads[:4] + st_loads + loads[4:]:
        copy.start()

    pl.semaphore_wait(barrier, n)
    own.wait()

    def to_chip(src, dst, step, send, recv):
        return pltpu.make_async_remote_copy(
            src_ref=src, dst_ref=dst, send_sem=send, recv_sem=recv,
            device_id={"kv": lax.rem(kv + step, n)}, device_id_type=MESH,
        )

    def to_sibling(ref, send, recv):
        return pltpu.make_async_remote_copy(
            src_ref=ref, dst_ref=ref, send_sem=send, recv_sem=recv,
            device_id={"tp": other}, device_id_type=MESH,
        )

    order = sorted(range(1, n), key=lambda step: (min(step, n - step), step))
    first = {}
    for step in order:
        first[step] = to_chip(
            xg.at[0, tp], xg.at[n - step, tp], step, s1.at[step], r1.at[n - step]
        )
        first[step].start()
    first_sib = {0: to_sibling(xg.at[0, tp], s1b.at[0], r1b.at[0])}
    first_sib[0].start()

    eye = (
        lax.broadcasted_iota(jnp.int32, (seqs, seqs), 0)
        == lax.broadcasted_iota(jnp.int32, (seqs, seqs), 1)
    ).astype(F32)

    def turn(value):
        return lax.dot_general(eye, value, NT, precision=HIGH, preferred_element_type=F32)

    parent = turn(pred_ref[...].astype(F32))
    admitted = turn(adm_ref[...].astype(F32))[:, :1]
    current = [jnp.full((seqs, 1), float(j), F32) for j in range(props)]
    above = [parent[:, j : j + 1] for j in range(props)]
    onehot = {}
    depth = [jnp.zeros((seqs, 1), F32) for _ in range(props)]
    lineage = {}
    for lag in range(props):
        for j in range(props):
            for i in range(j + 1):
                onehot[lag, j, i] = (current[j] == float(i)).astype(F32)
                lineage[j, i] = lineage.get((j, i), 0.0) + onehot[lag, j, i]
            if lag > 0:
                depth[j] = depth[j] + (current[j] >= 0.0).astype(F32)
        for j in range(props):
            upward = jnp.full((seqs, 1), -1.0, F32)
            for i in range(j + 1):
                hit = onehot[lag, j, i]
                upward = upward + hit * (above[i] + 1.0)
            current[j] = upward
    depth_is = {
        (j, d): (depth[j] == float(d)).astype(F32) for j in range(props) for d in range(j + 1)
    }
    slots = xsave_ref.shape[0]
    pick = [(admitted == float(a)).astype(F32) for a in range(slots - CONV + 2)]

    def previous(save):
        return [
            sum(pick[a] * save(a + back) for a in range(len(pick)))
            for back in range(CONV - 1)
        ]

    def conv(slabs, prev, tap):
        result = []
        for j in range(props):
            total = tap(CONV - 1) * slabs[j]
            for lag in range(1, CONV):
                value = None
                for i in range(j - lag + 1):
                    term = onehot[lag, j, i] * slabs[i]
                    value = term if value is None else value + term
                for d in range(min(lag, j + 1)):
                    term = depth_is[j, d] * prev[CONV - 1 - lag + d]
                    value = term if value is None else value + term
                total = total + tap(CONV - 1 - lag) * value
            result.append(silu(total))
        return result

    for copy in loads[:4]:
        copy.wait()
    squares = jnp.zeros((rows, 1), F32)
    acc_b = jnp.zeros((rows, wb.shape[1]), F32)
    acc_c = jnp.zeros((rows, wc.shape[1]), F32)
    acc_dt = jnp.zeros((rows, heads), F32)
    for place, slot in enumerate([0] + [n - step for step in order]):
        if slot:
            to_chip(xg.at[0, tp], xg.at[slot, tp], 1, s1.at[0], r1.at[slot]).wait_recv()
            first_sib[slot] = to_sibling(xg.at[slot, tp], s1b.at[slot], r1b.at[slot])
            first_sib[slot].start()
        to_sibling(xg.at[slot, other], s1b.at[slot], r1b.at[slot]).wait_recv()
        chip = lax.rem(kv + slot, n)
        base = pl.multiple_of(chip * (2 * feat), 2 * feat)
        tokens = jnp.concatenate([xg[slot, 0], xg[slot, 1]], axis=1).astype(F32)
        squares = squares + jnp.sum(tokens * tokens, axis=1, keepdims=True)
        span_k = pl.ds(base, 2 * feat)
        scaled = (tokens * gain_ref[:, span_k].astype(F32)).astype(BF16)
        px = lax.dot_general(scaled, wx[:, span_k], NT, preferred_element_type=F32)
        pz = lax.dot_general(scaled, wz[:, span_k], NT, preferred_element_type=F32)
        if place == 0:
            acc_x[...] = px
            acc_z[...] = pz
        else:
            acc_x[...] += px
            acc_z[...] += pz
        acc_b = acc_b + jnp.dot(scaled, wb[span_k, :], preferred_element_type=F32)
        acc_c = acc_c + jnp.dot(scaled, wc[span_k, :], preferred_element_type=F32)
        acc_dt = acc_dt + lax.dot_general(
            scaled, dtw_ref[:, span_k], NT, preferred_element_type=F32
        )
    r_in = lax.rsqrt(squares / d_model + 1e-06)

    def slabs_of(value):
        return [value[j * seqs : (j + 1) * seqs] for j in range(props)]

    def rounded(value):
        return value.astype(BF16).astype(F32)

    b_conv = conv(
        slabs_of(rounded(acc_b * r_in)),
        previous(lambda w: bsave_ref[w].astype(F32)),
        lambda k: btap_ref[k],
    )
    c_conv = conv(
        slabs_of(rounded(acc_c * r_in)),
        previous(lambda w: csave_ref[w].astype(F32)),
        lambda k: ctap_ref[k],
    )
    for j in range(props):
        cs[pl.ds(j, seqs, stride=props), :] = c_conv[j]

    raw = acc_dt * r_in + offset_ref[...]
    step_size = slabs_of(jnp.maximum(raw, 0.0) + jnp.log1p(jnp.exp(-jnp.abs(raw))))
    rate = jnp.exp(shrink_ref[...])
    fade = [turn(fade_ref[j]) - rate * step_size[j] for j in range(props)]
    level = [
        sum(lineage[j, i] * fade[i] for i in range(j + 1)) for j in range(props)
    ]
    pairs = [(j, i) for j in range(props) for i in range(j + 1)]
    table = []
    for j, i in pairs:
        score = jnp.sum(c_conv[j] * b_conv[i], axis=1, keepdims=True)
        table.append(
            lineage[j, i] * jnp.exp(jnp.minimum(level[j] - level[i], 0.0)) * score * step_size[i]
            + (bypass_ref[...] if i == j else 0.0)
        )
    table += [jnp.exp(level[j]) for j in range(props)]
    table = jnp.concatenate(table, axis=0)
    table_hi = table.astype(BF16)
    table_lo = (table - table_hi.astype(F32)).astype(BF16)

    for copy in st_loads:
        copy.wait()
    pack = 8 // props
    order2 = order
    second = {}
    second_sib = {}
    lanes = 128
    for ch in range(chunks):
        cols = slice(ch * cw, (ch + 1) * cw)

        def group(g, carry):
            at = pl.multiple_of(g * 8, 8)
            reads = cs[pl.ds(at, 8), :].astype(BF16)
            row = lax.broadcasted_iota(jnp.int32, (8, cw), 0)
            total = None
            for k in range(pack):
                state = st[g * pack + k, ch * cw : (ch + 1) * cw, :].astype(BF16)
                part = lax.dot_general(reads, state, NT, preferred_element_type=F32)
                total = part if total is None else jnp.where(row < k * props, total, part)
            for lane in range(cw // lanes):
                ys[lane, pl.ds(at, 8), :] = total[:, lane * lanes : (lane + 1) * lanes]
            return carry

        def block(q, carry):
            for k in range(4):
                group(q * 4 + k, 0)
            return carry

        lax.fori_loop(0, seqs // pack // 4, block, 0)

        spread = (
            lax.broadcasted_iota(jnp.int32, (heads, cw), 0)
            == (lax.broadcasted_iota(jnp.int32, (heads, cw), 1) + ch * cw) // hd
        ).astype(BF16)
        mix = jnp.dot(table_hi, spread, preferred_element_type=F32) + jnp.dot(
            table_lo, spread, preferred_element_type=F32
        )
        x_conv = conv(
            slabs_of(rounded(acc_x[:, cols] * r_in)),
            previous(lambda w: xsave_ref[w, :, cols].astype(F32)),
            lambda k: xtap_ref[k : k + 1, cols],
        )
        gate = slabs_of(silu(rounded(acc_z[:, cols] * r_in)))
        for j in range(props):
            carried = jnp.concatenate(
                [ys[lane, pl.ds(j, seqs, stride=props), :] for lane in range(cw // lanes)], axis=1
            )
            at = (len(pairs) + j) * seqs
            y = mix[at : at + seqs] * carried
            for index, (to, i) in enumerate(pairs):
                if to == j:
                    y = y + mix[index * seqs : (index + 1) * seqs] * x_conv[i]
            gg[0, tp, ch, pl.ds(j * seqs, seqs), :] = (y * gate[j]).astype(BF16)
        for step in order2:
            second[step, ch] = to_chip(
                gg.at[0, tp, ch], gg.at[n - step, tp, ch], step,
                s2.at[step, ch], r2.at[n - step, ch],
            )
            second[step, ch].start()
        second_sib[0, ch] = to_sibling(gg.at[0, tp, ch], s2b.at[0, ch], r2b.at[0, ch])
        second_sib[0, ch].start()

    loads[4].wait()
    product = jnp.zeros((rows, fl.shape[3]), F32)
    total_sq = jnp.zeros((rows, 1), F32)

    def add_piece(product, total_sq, slot, core, ch):
        value = gg[slot, core, ch]
        chip = lax.rem(kv + slot, n)
        weight = fl[pl.ds(chip * heads + ch * hpc, hpc), core].reshape(cw, fl.shape[3])
        product = product + jnp.dot(value, weight, preferred_element_type=F32)
        value = value.astype(F32)
        return product, total_sq + jnp.sum(value * value, axis=1, keepdims=True)

    for ch in range(chunks):
        product, total_sq = add_piece(product, total_sq, 0, tp, ch)
    for ch in range(chunks):
        to_sibling(gg.at[0, other, ch], s2b.at[0, ch], r2b.at[0, ch]).wait_recv()
        product, total_sq = add_piece(product, total_sq, 0, other, ch)
    arrivals = [(n - step, ch) for step in order for ch in range(chunks)]
    for slot, ch in arrivals:
        to_chip(
            gg.at[0, tp, ch], gg.at[slot, tp, ch], 1, s2.at[0, ch], r2.at[slot, ch]
        ).wait_recv()
        second_sib[slot, ch] = to_sibling(gg.at[slot, tp, ch], s2b.at[slot, ch], r2b.at[slot, ch])
        second_sib[slot, ch].start()
        product, total_sq = add_piece(product, total_sq, slot, tp, ch)
        to_sibling(gg.at[slot, other, ch], s2b.at[slot, ch], r2b.at[slot, ch]).wait_recv()
        product, total_sq = add_piece(product, total_sq, slot, other, ch)
    r_out = lax.rsqrt(total_sq / (heads_all * hd) + 1e-05)
    out_ref[...] = (product * r_out).astype(BF16)
    for copy in list(first.values()) + list(first_sib.values()):
        copy.wait_send()
    for copy in list(second.values()) + list(second_sib.values()):
        copy.wait_send()


def shards(
    candidate_vectors,
    leading_scaling_factor,
    lane_feed_matrix,
    final_valve_matrix,
    increment_matrix,
    entry_basis_matrix,
    readout_basis_matrix,
    lane_feed_kernel,
    entry_basis_kernel,
    readout_basis_kernel,
    increment_offset,
    shrink_speed_exponent,
    lane_bypass_factor,
    final_linear_matrix,
    hidden_carried_memory,
    lane_filter_memory,
    entry_basis_memory,
    readout_basis_memory,
    predecessor_index,
    admitted_counts,
    surplus_fading,
):
    seqs, props, feat = candidate_vectors.shape
    heads = increment_offset.shape[0]
    hd = lane_feed_matrix.shape[3]
    d_model = lane_feed_matrix.shape[0]
    state = hidden_carried_memory.shape[4]
    window = lane_filter_memory.shape[1]
    heads_all, groups, _, out_cols = final_linear_matrix.shape
    n = lax.axis_size("kv")
    rows = seqs * props
    wide = heads * hd
    chunks = max(1, wide // 256)
    cw = wide // chunks
    x = candidate_vectors.transpose(1, 0, 2).reshape(rows, feat)
    wx = lane_feed_matrix.transpose(1, 2, 3, 0).reshape(wide, d_model)
    wz = final_valve_matrix.transpose(1, 2, 3, 0).reshape(wide, d_model)
    dtw = lax.dynamic_slice(
        increment_matrix.transpose(1, 2, 0),
        (lax.axis_index("kv") * heads, lax.axis_index("tp"), 0),
        (heads, 1, d_model),
    ).reshape(heads, d_model)
    wb = entry_basis_matrix.reshape(d_model, state)
    wc = readout_basis_matrix.reshape(d_model, state)
    xsave = (
        lane_filter_memory.reshape(seqs, window, heads, hd)
        .transpose(1, 0, 2, 3)
        .reshape(window, seqs, wide)
    )
    args = (
        x,
        leading_scaling_factor.reshape(1, d_model),
        wx,
        wz,
        dtw,
        wb,
        wc,
        lane_feed_kernel.reshape(CONV, wide),
        entry_basis_kernel,
        readout_basis_kernel,
        increment_offset.reshape(1, heads),
        shrink_speed_exponent.reshape(1, heads),
        lane_bypass_factor.reshape(1, heads),
        final_linear_matrix,
        hidden_carried_memory.reshape(seqs, wide, state),
        xsave,
        entry_basis_memory.transpose(1, 2, 0, 3).reshape(window, seqs, state),
        readout_basis_memory.transpose(1, 2, 0, 3).reshape(window, seqs, state),
        predecessor_index.T,
        admitted_counts.reshape(1, seqs),
        surplus_fading.transpose(1, 2, 3, 0).reshape(props, heads, seqs),
    )
    in_hbm = {0, 2, 3, 5, 6, 13, 14}
    vmem = pl.BlockSpec(memory_space=pltpu.VMEM)
    anywhere = pl.BlockSpec(memory_space=pl.ANY)
    dma = pltpu.SemaphoreType.DMA
    mixed = pl.pallas_call(
        functools.partial(
            mixer_kernel, n, seqs, props, heads, hd, chunks, d_model, heads_all * groups
        ),
        out_shape=jax.ShapeDtypeStruct((rows, out_cols), BF16),
        in_specs=[anywhere if k in in_hbm else vmem for k in range(len(args))],
        out_specs=vmem,
        scratch_shapes=[
            pltpu.VMEM((n, 2, rows, feat), BF16),
            pltpu.VMEM((n, 2, chunks, rows, cw), BF16),
            pltpu.VMEM((wide, d_model), BF16),
            pltpu.VMEM((wide, d_model), BF16),
            pltpu.VMEM((d_model, state), BF16),
            pltpu.VMEM((d_model, state), BF16),
            pltpu.VMEM(final_linear_matrix.shape, BF16),
            pltpu.VMEM((seqs, wide, state), F32),
            pltpu.VMEM((rows, wide), F32),
            pltpu.VMEM((rows, wide), F32),
            pltpu.VMEM((8, 128), F32),
            pltpu.VMEM((rows, state), F32),
            pltpu.VMEM((cw // 128, rows, 128), F32),
            dma((5,)),
            dma((4,)),
            dma,
            dma((n,)),
            dma((n,)),
            dma((n,)),
            dma((n,)),
            dma((n, chunks)),
            dma((n, chunks)),
            dma((n, chunks)),
            dma((n, chunks)),
        ],
        compiler_params=pltpu.CompilerParams(collective_id=0, has_side_effects=True),
    )(*args)
    return mixed.reshape(props, seqs, out_cols).transpose(1, 0, 2)


def solution(mesh):
    placed = (
        P(("grp", "dp"), None, ("kv", "tp")),
        P(),
        P(None, "kv", "tp", None),
        P(None, "kv", "tp", None),
        P(),
        P(None, "tp", None),
        P(None, "tp", None),
        P(None, "kv", "tp", None),
        P(None, "tp", None),
        P(None, "tp", None),
        P("kv", "tp"),
        P("kv", "tp"),
        P("kv", "tp"),
        P(None, None, None, ("kv", "tp")),
        P(("grp", "dp"), "kv", "tp", None, None),
        P(("grp", "dp"), None, "kv", "tp", None),
        P(("grp", "dp"), None, "tp", None),
        P(("grp", "dp"), None, "tp", None),
        P(("grp", "dp"), None),
        P(("grp", "dp")),
        P(("grp", "dp"), None, "kv", "tp"),
    )
    return jax.shard_map(
        shards,
        mesh=mesh,
        in_specs=placed,
        out_specs=P(("grp", "dp"), None, ("kv", "tp")),
        check_vma=False,
    )
```

```python
import functools

import jax
import jax.numpy as jnp
from jax import lax
from jax.experimental import pallas as pl
from jax.experimental.pallas import tpu as pltpu
from jax.sharding import PartitionSpec as P

CONV = 4
MESH = pl.DeviceIdType.MESH
HIGH = lax.Precision.HIGHEST
F32 = jnp.float32
BF16 = jnp.bfloat16
NT = (((1,), (1,)), ((), ()))


def silu(value):
    return value * jax.nn.sigmoid(value)


def mixer_kernel(
    n, seqs, props, heads, hd, chunks, d_model, heads_all,
    x_hbm, gain_ref, wx_hbm, wz_hbm, inc_hbm, wb_hbm, wc_hbm,
    xtap_ref, btap_ref, ctap_ref, offset_ref, shrink_ref, bypass_ref,
    fl_hbm, st_hbm, xsave_hbm, bsave_ref, csave_ref, pred_ref, adm_ref, slot_ref, fade_ref,
    out_ref,
    xg, gg, wx, wz, wb, wc, fl, st, acc_x, acc_z, cs, ys,
    xin, xrow, gain, inc, inc_rows, dtw, xsave, xprev,
    load_sem, st_sem, own_sem, s1, r1, s1b, r1b, s2, r2, s2b, r2b,
):
    kv = lax.axis_index("kv")
    tp = lax.axis_index("tp")
    other = 1 - tp
    rows = seqs * props
    feat = x_hbm.shape[2]
    lanes = 128
    wide = heads * hd
    cw = wide // chunks
    hpc = heads // chunks

    own = pltpu.make_async_copy(x_hbm, xin, own_sem)
    own.start()
    barrier = pltpu.get_barrier_semaphore()
    for step in range(1, n):
        pl.semaphore_signal(
            barrier, inc=1, device_id={"kv": lax.rem(kv + step, n)}, device_id_type=MESH
        )
    pl.semaphore_signal(barrier, inc=1, device_id={"tp": other}, device_id_type=MESH)

    loads = []
    for index, (src, dst) in enumerate(
        (
            (wb_hbm, wb),
            (wc_hbm, wc),
            (wx_hbm, wx),
            (wz_hbm, wz),
            (inc_hbm.at[pl.ds(kv * heads, heads)], inc),
            (xsave_hbm, xsave),
            (fl_hbm, fl),
        )
    ):
        loads.append(pltpu.make_async_copy(src, dst, load_sem.at[index]))
    parts = st_sem.shape[0]
    span = seqs // parts
    st_loads = [
        pltpu.make_async_copy(
            st_hbm.at[pl.ds(part * span, span)], st.at[pl.ds(part * span, span)], st_sem.at[part]
        )
        for part in range(parts)
    ]
    for copy in loads[:6] + st_loads + loads[6:]:
        copy.start()

    own.wait()
    tiles = xrow.shape[0]
    tile_w = feat // tiles
    for s in range(seqs):
        for tile in range(tiles):
            xrow[tile, s * props : (s + 1) * props, :tile_w] = xin[
                s, :, tile * tile_w : (tile + 1) * tile_w
            ].astype(F32)
    for j in range(props):
        for tile in range(tiles):
            xg[0, tp, j * seqs : (j + 1) * seqs, tile * tile_w : (tile + 1) * tile_w] = xrow[
                tile, pl.ds(j, seqs, stride=props), :
            ][:, :tile_w].astype(BF16)
    pl.semaphore_wait(barrier, n)

    def to_chip(src, dst, step, send, recv):
        return pltpu.make_async_remote_copy(
            src_ref=src, dst_ref=dst, send_sem=send, recv_sem=recv,
            device_id={"kv": lax.rem(kv + step, n)}, device_id_type=MESH,
        )

    def to_sibling(ref, send, recv):
        return pltpu.make_async_remote_copy(
            src_ref=ref, dst_ref=ref, send_sem=send, recv_sem=recv,
            device_id={"tp": other}, device_id_type=MESH,
        )

    order = sorted(range(1, n), key=lambda step: (min(step, n - step), step))
    first = {}
    for step in order:
        first[step] = to_chip(
            xg.at[0, tp], xg.at[n - step, tp], step, s1.at[step], r1.at[n - step]
        )
        first[step].start()
    first_sib = {0: to_sibling(xg.at[0, tp], s1b.at[0], r1b.at[0])}
    first_sib[0].start()

    eye = (
        lax.broadcasted_iota(jnp.int32, (seqs, seqs), 0)
        == lax.broadcasted_iota(jnp.int32, (seqs, seqs), 1)
    ).astype(F32)

    def turn(value):
        return lax.dot_general(eye, value, NT, precision=HIGH, preferred_element_type=F32)

    parent = turn(pred_ref[...].astype(F32))
    admitted = turn(adm_ref[...].astype(F32))[:, :1]
    current = [jnp.full((seqs, 1), float(j), F32) for j in range(props)]
    above = [parent[:, j : j + 1] for j in range(props)]
    onehot = {}
    depth = [jnp.zeros((seqs, 1), F32) for _ in range(props)]
    lineage = {}
    for lag in range(props):
        for j in range(props):
            for i in range(j + 1):
                onehot[lag, j, i] = (current[j] == float(i)).astype(F32)
                lineage[j, i] = lineage.get((j, i), 0.0) + onehot[lag, j, i]
            if lag > 0:
                depth[j] = depth[j] + (current[j] >= 0.0).astype(F32)
        for j in range(props):
            upward = jnp.full((seqs, 1), -1.0, F32)
            for i in range(j + 1):
                hit = onehot[lag, j, i]
                upward = upward + hit * (above[i] + 1.0)
            current[j] = upward
    depth_is = {
        (j, d): (depth[j] == float(d)).astype(F32) for j in range(props) for d in range(j + 1)
    }
    slots = bsave_ref.shape[0]
    pick = [(admitted == float(a)).astype(F32) for a in range(slots - CONV + 2)]

    def previous(save):
        return [
            sum(pick[a] * save(a + back) for a in range(len(pick)))
            for back in range(CONV - 1)
        ]

    def conv(slabs, prev, tap):
        result = []
        for j in range(props):
            total = tap(CONV - 1) * slabs[j]
            for lag in range(1, CONV):
                value = None
                for i in range(j - lag + 1):
                    term = onehot[lag, j, i] * slabs[i]
                    value = term if value is None else value + term
                for d in range(min(lag, j + 1)):
                    term = depth_is[j, d] * prev[CONV - 1 - lag + d]
                    value = term if value is None else value + term
                total = total + tap(CONV - 1 - lag) * value
            result.append(silu(total))
        return result

    for copy in loads[:6]:
        copy.wait()
    gain[...] = gain_ref[...].astype(F32)
    for h in range(heads):
        inc_rows[2 * h : 2 * h + 2, :] = inc[h].astype(F32)
    dtw[...] = inc_rows[...].astype(BF16)

    def pick_rows(block, carry):
        for k in range(4):
            s = block * 4 + k
            for back in range(CONV - 1):
                at = pl.multiple_of(s * heads, heads)
                xprev[back, pl.ds(at, heads), :hd] = xsave[s, slot_ref[s] + back].astype(F32)
        return carry

    lax.fori_loop(0, seqs // 4, pick_rows, 0)
    squares = jnp.zeros((rows, 1), F32)
    acc_b = jnp.zeros((rows, wb.shape[1]), F32)
    acc_c = jnp.zeros((rows, wc.shape[1]), F32)
    acc_dt = jnp.zeros((rows, 2 * heads), F32)
    for place, slot in enumerate([0] + [n - step for step in order]):
        if slot:
            to_chip(xg.at[0, tp], xg.at[slot, tp], 1, s1.at[0], r1.at[slot]).wait_recv()
            first_sib[slot] = to_sibling(xg.at[slot, tp], s1b.at[slot], r1b.at[slot])
            first_sib[slot].start()
        to_sibling(xg.at[slot, other], s1b.at[slot], r1b.at[slot]).wait_recv()
        chip = lax.rem(kv + slot, n)
        base = pl.multiple_of(chip * (2 * feat), 2 * feat)
        tokens = jnp.concatenate([xg[slot, 0], xg[slot, 1]], axis=1).astype(F32)
        squares = squares + jnp.sum(tokens * tokens, axis=1, keepdims=True)
        span_k = pl.ds(base, 2 * feat)
        gain_rows = 2 * feat // lanes
        gains = jnp.concatenate(
            [gain[pl.ds(chip * gain_rows + k, 1), :] for k in range(gain_rows)], axis=1
        )
        scaled = (tokens * gains).astype(BF16)
        px = lax.dot_general(scaled, wx[:, span_k], NT, preferred_element_type=F32)
        pz = lax.dot_general(scaled, wz[:, span_k], NT, preferred_element_type=F32)
        if place == 0:
            acc_x[...] = px
            acc_z[...] = pz
        else:
            acc_x[...] += px
            acc_z[...] += pz
        acc_b = acc_b + jnp.dot(scaled, wb[span_k, :], preferred_element_type=F32)
        acc_c = acc_c + jnp.dot(scaled, wc[span_k, :], preferred_element_type=F32)
        acc_dt = acc_dt + lax.dot_general(
            scaled, dtw[:, span_k], NT, preferred_element_type=F32
        )
    r_in = lax.rsqrt(squares / d_model + 1e-06)

    def slabs_of(value):
        return [value[j * seqs : (j + 1) * seqs] for j in range(props)]

    def rounded(value):
        return value.astype(BF16).astype(F32)

    b_conv = conv(
        slabs_of(rounded(acc_b * r_in)),
        previous(lambda w: bsave_ref[w].astype(F32)),
        lambda k: btap_ref[k],
    )
    c_conv = conv(
        slabs_of(rounded(acc_c * r_in)),
        previous(lambda w: csave_ref[w].astype(F32)),
        lambda k: ctap_ref[k],
    )
    for j in range(props):
        cs[pl.ds(j, seqs, stride=props), :] = c_conv[j]

    mine = (
        lax.broadcasted_iota(jnp.int32, (2 * heads, heads), 0)
        == 2 * lax.broadcasted_iota(jnp.int32, (2 * heads, heads), 1) + tp
    ).astype(F32)
    acc_dt = jnp.dot(acc_dt, mine, precision=HIGH, preferred_element_type=F32)
    raw = acc_dt * r_in + offset_ref[...]
    step_size = slabs_of(jnp.maximum(raw, 0.0) + jnp.log1p(jnp.exp(-jnp.abs(raw))))
    rate = jnp.exp(shrink_ref[...])
    fade = [turn(fade_ref[j]) - rate * step_size[j] for j in range(props)]
    level = [
        sum(lineage[j, i] * fade[i] for i in range(j + 1)) for j in range(props)
    ]
    pairs = [(j, i) for j in range(props) for i in range(j + 1)]
    table = []
    for j, i in pairs:
        score = jnp.sum(c_conv[j] * b_conv[i], axis=1, keepdims=True)
        table.append(
            lineage[j, i] * jnp.exp(jnp.minimum(level[j] - level[i], 0.0)) * score * step_size[i]
            + (bypass_ref[...] if i == j else 0.0)
        )
    table += [jnp.exp(level[j]) for j in range(props)]
    table = jnp.concatenate(table, axis=0)
    table_hi = table.astype(BF16)
    table_lo = (table - table_hi.astype(F32)).astype(BF16)

    for copy in st_loads:
        copy.wait()
    pack = 8 // props
    order2 = order
    second = {}
    second_sib = {}
    for ch in range(chunks):
        cols = slice(ch * cw, (ch + 1) * cw)

        def group(g, carry):
            at = pl.multiple_of(g * 8, 8)
            reads = cs[pl.ds(at, 8), :].astype(BF16)
            row = lax.broadcasted_iota(jnp.int32, (8, cw), 0)
            total = None
            for k in range(pack):
                state = st[g * pack + k, ch * cw : (ch + 1) * cw, :].astype(BF16)
                part = lax.dot_general(reads, state, NT, preferred_element_type=F32)
                total = part if total is None else jnp.where(row < k * props, total, part)
            for lane in range(cw // lanes):
                ys[lane, pl.ds(at, 8), :] = total[:, lane * lanes : (lane + 1) * lanes]
            return carry

        def block(q, carry):
            for k in range(4):
                group(q * 4 + k, 0)
            return carry

        lax.fori_loop(0, seqs // pack // 4, block, 0)

        spread = (
            lax.broadcasted_iota(jnp.int32, (heads, cw), 0)
            == (lax.broadcasted_iota(jnp.int32, (heads, cw), 1) + ch * cw) // hd
        ).astype(BF16)
        mix = jnp.dot(table_hi, spread, preferred_element_type=F32) + jnp.dot(
            table_lo, spread, preferred_element_type=F32
        )
        x_conv = conv(
            slabs_of(rounded(acc_x[:, cols] * r_in)),
            [
                jnp.concatenate(
                    [
                        xprev[back, pl.ds(ch * hpc + h, seqs, stride=heads), :][:, :hd]
                        for h in range(hpc)
                    ],
                    axis=1,
                )
                for back in range(CONV - 1)
            ],
            lambda k: jnp.concatenate(
                [xtap_ref[k, ch * hpc + h] for h in range(hpc)], axis=1
            ),
        )
        gate = slabs_of(silu(rounded(acc_z[:, cols] * r_in)))
        for j in range(props):
            carried = jnp.concatenate(
                [ys[lane, pl.ds(j, seqs, stride=props), :] for lane in range(cw // lanes)], axis=1
            )
            at = (len(pairs) + j) * seqs
            y = mix[at : at + seqs] * carried
            for index, (to, i) in enumerate(pairs):
                if to == j:
                    y = y + mix[index * seqs : (index + 1) * seqs] * x_conv[i]
            gg[0, tp, ch, pl.ds(j * seqs, seqs), :] = (y * gate[j]).astype(BF16)
        for step in order2:
            second[step, ch] = to_chip(
                gg.at[0, tp, ch], gg.at[n - step, tp, ch], step,
                s2.at[step, ch], r2.at[n - step, ch],
            )
            second[step, ch].start()
        second_sib[0, ch] = to_sibling(gg.at[0, tp, ch], s2b.at[0, ch], r2b.at[0, ch])
        second_sib[0, ch].start()

    loads[6].wait()
    product = jnp.zeros((rows, fl.shape[3]), F32)
    total_sq = jnp.zeros((rows, 1), F32)

    def add_piece(product, total_sq, slot, core, ch):
        value = gg[slot, core, ch]
        chip = lax.rem(kv + slot, n)
        weight = fl[pl.ds(chip * heads + ch * hpc, hpc), core].reshape(cw, fl.shape[3])
        product = product + jnp.dot(value, weight, preferred_element_type=F32)
        value = value.astype(F32)
        return product, total_sq + jnp.sum(value * value, axis=1, keepdims=True)

    for ch in range(chunks):
        product, total_sq = add_piece(product, total_sq, 0, tp, ch)
    for ch in range(chunks):
        to_sibling(gg.at[0, other, ch], s2b.at[0, ch], r2b.at[0, ch]).wait_recv()
        product, total_sq = add_piece(product, total_sq, 0, other, ch)
    arrivals = [(n - step, ch) for step in order for ch in range(chunks)]
    for slot, ch in arrivals:
        to_chip(
            gg.at[0, tp, ch], gg.at[slot, tp, ch], 1, s2.at[0, ch], r2.at[slot, ch]
        ).wait_recv()
        second_sib[slot, ch] = to_sibling(gg.at[slot, tp, ch], s2b.at[slot, ch], r2b.at[slot, ch])
        second_sib[slot, ch].start()
        product, total_sq = add_piece(product, total_sq, slot, tp, ch)
        to_sibling(gg.at[slot, other, ch], s2b.at[slot, ch], r2b.at[slot, ch]).wait_recv()
        product, total_sq = add_piece(product, total_sq, slot, other, ch)
    r_out = lax.rsqrt(total_sq / (heads_all * hd) + 1e-05)
    out_ref[...] = (product * r_out).astype(BF16)
    for copy in list(first.values()) + list(first_sib.values()):
        copy.wait_send()
    for copy in list(second.values()) + list(second_sib.values()):
        copy.wait_send()


def shards(
    candidate_vectors,
    leading_scaling_factor,
    lane_feed_matrix,
    final_valve_matrix,
    increment_matrix,
    entry_basis_matrix,
    readout_basis_matrix,
    lane_feed_kernel,
    entry_basis_kernel,
    readout_basis_kernel,
    increment_offset,
    shrink_speed_exponent,
    lane_bypass_factor,
    final_linear_matrix,
    hidden_carried_memory,
    lane_filter_memory,
    entry_basis_memory,
    readout_basis_memory,
    predecessor_index,
    admitted_counts,
    surplus_fading,
):
    seqs, props, feat = candidate_vectors.shape
    heads = increment_offset.shape[0]
    hd = lane_feed_matrix.shape[3]
    d_model = lane_feed_matrix.shape[0]
    state = hidden_carried_memory.shape[4]
    window = lane_filter_memory.shape[1]
    heads_all, groups, _, out_cols = final_linear_matrix.shape
    n = lax.axis_size("kv")
    rows = seqs * props
    wide = heads * hd
    chunks = max(1, wide // 256)
    cw = wide // chunks
    wx = lane_feed_matrix.transpose(1, 2, 3, 0).reshape(wide, d_model)
    wz = final_valve_matrix.transpose(1, 2, 3, 0).reshape(wide, d_model)
    wb = entry_basis_matrix.reshape(d_model, state)
    wc = readout_basis_matrix.reshape(d_model, state)
    args = (
        candidate_vectors,
        leading_scaling_factor.reshape(d_model // 128, 128),
        wx,
        wz,
        increment_matrix.transpose(1, 2, 0),
        wb,
        wc,
        lane_feed_kernel,
        entry_basis_kernel,
        readout_basis_kernel,
        increment_offset.reshape(1, heads),
        shrink_speed_exponent.reshape(1, heads),
        lane_bypass_factor.reshape(1, heads),
        final_linear_matrix,
        hidden_carried_memory.reshape(seqs, wide, state),
        lane_filter_memory.reshape(seqs, window, heads, hd),
        entry_basis_memory.transpose(1, 2, 0, 3).reshape(window, seqs, state),
        readout_basis_memory.transpose(1, 2, 0, 3).reshape(window, seqs, state),
        predecessor_index.T,
        admitted_counts.reshape(1, seqs),
        admitted_counts,
        surplus_fading.transpose(1, 2, 3, 0).reshape(props, heads, seqs),
    )
    in_hbm = {0, 2, 3, 4, 5, 6, 13, 14, 15}
    in_smem = 20
    vmem = pl.BlockSpec(memory_space=pltpu.VMEM)
    anywhere = pl.BlockSpec(memory_space=pl.ANY)
    scalars = pl.BlockSpec(memory_space=pltpu.SMEM)
    dma = pltpu.SemaphoreType.DMA
    tiles = max(1, feat // 128)
    mixed = pl.pallas_call(
        functools.partial(
            mixer_kernel, n, seqs, props, heads, hd, chunks, d_model, heads_all * groups
        ),
        out_shape=jax.ShapeDtypeStruct((rows, out_cols), BF16),
        in_specs=[
            anywhere if k in in_hbm else scalars if k == in_smem else vmem
            for k in range(len(args))
        ],
        out_specs=vmem,
        scratch_shapes=[
            pltpu.VMEM((n, 2, rows, feat), BF16),
            pltpu.VMEM((n, 2, chunks, rows, cw), BF16),
            pltpu.VMEM((wide, d_model), BF16),
            pltpu.VMEM((wide, d_model), BF16),
            pltpu.VMEM((d_model, state), BF16),
            pltpu.VMEM((d_model, state), BF16),
            pltpu.VMEM(final_linear_matrix.shape, BF16),
            pltpu.VMEM((seqs, wide, state), F32),
            pltpu.VMEM((rows, wide), F32),
            pltpu.VMEM((rows, wide), F32),
            pltpu.VMEM((rows, state), F32),
            pltpu.VMEM((cw // 128, rows, 128), F32),
            pltpu.VMEM((seqs, props, feat), BF16),
            pltpu.VMEM((tiles, rows, 128), F32),
            pltpu.VMEM((d_model // 128, 128), F32),
            pltpu.VMEM((heads, groups, d_model), BF16),
            pltpu.VMEM((heads * groups, d_model), F32),
            pltpu.VMEM((heads * groups, d_model), BF16),
            pltpu.VMEM((seqs, window, heads, hd), BF16),
            pltpu.VMEM((CONV - 1, seqs * heads, 128), F32),
            dma((7,)),
            dma((4,)),
            dma,
            dma((n,)),
            dma((n,)),
            dma((n,)),
            dma((n,)),
            dma((n, chunks)),
            dma((n, chunks)),
            dma((n, chunks)),
            dma((n, chunks)),
        ],
        compiler_params=pltpu.CompilerParams(collective_id=0, has_side_effects=True),
    )(*args)
    return mixed.reshape(props, seqs, out_cols).transpose(1, 0, 2)


def solution(mesh):
    placed = (
        P(("grp", "dp"), None, ("kv", "tp")),
        P(),
        P(None, "kv", "tp", None),
        P(None, "kv", "tp", None),
        P(),
        P(None, "tp", None),
        P(None, "tp", None),
        P(None, "kv", "tp", None),
        P(None, "tp", None),
        P(None, "tp", None),
        P("kv", "tp"),
        P("kv", "tp"),
        P("kv", "tp"),
        P(None, None, None, ("kv", "tp")),
        P(("grp", "dp"), "kv", "tp", None, None),
        P(("grp", "dp"), None, "kv", "tp", None),
        P(("grp", "dp"), None, "tp", None),
        P(("grp", "dp"), None, "tp", None),
        P(("grp", "dp"), None),
        P(("grp", "dp")),
        P(("grp", "dp"), None, "kv", "tp"),
    )
    return jax.shard_map(
        shards,
        mesh=mesh,
        in_specs=placed,
        out_specs=P(("grp", "dp"), None, ("kv", "tp")),
        check_vma=False,
    )
```

```python
import functools

import jax
import jax.numpy as jnp
from jax import lax
from jax.experimental import pallas as pl
from jax.experimental.pallas import tpu as pltpu
from jax.sharding import PartitionSpec as P

CONV = 4
MESH = pl.DeviceIdType.MESH
HIGH = lax.Precision.HIGHEST
F32 = jnp.float32
BF16 = jnp.bfloat16
NT = (((1,), (1,)), ((), ()))


def silu(value):
    return value * jax.nn.sigmoid(value)


def mixer_kernel(
    n, seqs, props, heads, hd, chunks, d_model, heads_all,
    x_hbm, gain_ref, wx_hbm, wz_hbm, inc_hbm, wb_hbm, wc_hbm,
    xtap_ref, btap_ref, ctap_ref, offset_ref, shrink_ref, bypass_ref,
    fl_hbm, st_hbm, xsave_hbm, bsave_ref, csave_ref, pred_ref, adm_ref, slot_ref, fade_ref,
    out_ref,
    xg, gg, wx, wz, wb, wc, fl, st, acc_x, acc_z, cs, ys,
    xin, xrow, gain, inc, inc_rows, dtw, xsave, xprev,
    load_sem, st_sem, own_sem, s1, r1, s1b, r1b, s2, r2, s2b, r2b, p1, p2,
):
    kv = lax.axis_index("kv")
    tp = lax.axis_index("tp")
    other = 1 - tp
    rows = seqs * props
    feat = x_hbm.shape[2]
    lanes = 128
    wide = heads * hd
    cw = wide // chunks
    hpc = heads // chunks

    own = pltpu.make_async_copy(x_hbm, xin, own_sem)
    own.start()
    barrier = pltpu.get_barrier_semaphore()
    for step in range(1, n):
        pl.semaphore_signal(
            barrier, inc=1, device_id={"kv": lax.rem(kv + step, n)}, device_id_type=MESH
        )
    pl.semaphore_signal(barrier, inc=1, device_id={"tp": other}, device_id_type=MESH)

    loads = []
    for index, (src, dst) in enumerate(
        (
            (wb_hbm, wb),
            (wc_hbm, wc),
            (wx_hbm, wx),
            (wz_hbm, wz),
            (inc_hbm.at[pl.ds(kv * heads, heads)], inc),
            (xsave_hbm, xsave),
            (fl_hbm, fl),
        )
    ):
        loads.append(pltpu.make_async_copy(src, dst, load_sem.at[index]))
    parts = st_sem.shape[0]
    span = seqs // parts
    st_loads = [
        pltpu.make_async_copy(
            st_hbm.at[pl.ds(part * span, span)], st.at[pl.ds(part * span, span)], st_sem.at[part]
        )
        for part in range(parts)
    ]
    for copy in loads[:6] + st_loads + loads[6:]:
        copy.start()

    own.wait()
    tiles = xrow.shape[0]
    tile_w = feat // tiles
    for s in range(seqs):
        for tile in range(tiles):
            xrow[tile, s * props : (s + 1) * props, :tile_w] = xin[
                s, :, tile * tile_w : (tile + 1) * tile_w
            ].astype(F32)
    for j in range(props):
        for tile in range(tiles):
            xg[0, tp, j * seqs : (j + 1) * seqs, tile * tile_w : (tile + 1) * tile_w] = xrow[
                tile, pl.ds(j, seqs, stride=props), :
            ][:, :tile_w].astype(BF16)
    pl.semaphore_wait(barrier, n)

    def to_chip(src, dst, step, send, recv):
        return pltpu.make_async_remote_copy(
            src_ref=src, dst_ref=dst, send_sem=send, recv_sem=recv,
            device_id={"kv": lax.rem(kv + step, n)}, device_id_type=MESH,
        )

    def to_sibling(ref, send, recv):
        return pltpu.make_async_remote_copy(
            src_ref=ref, dst_ref=ref, send_sem=send, recv_sem=recv,
            device_id={"tp": other}, device_id_type=MESH,
        )

    relayed = n > 3

    def direct(step, action):
        if relayed and step == n - 1:
            pl.when(kv != 0)(action)
        elif relayed and step == 1:
            pl.when(kv != n - 1)(action)
        else:
            action()

    def passed(slot, view, send, recv):
        if not relayed:
            return []
        result = []
        if isinstance(slot, int) and slot == 2:
            result.append((kv == n - 2, to_chip(view(2), view(1), 1, send, recv(1))))
        if isinstance(slot, int) and slot == n - 2:
            result.append((kv == 1, to_chip(view(n - 2), view(n - 1), n - 1, send, recv(n - 1))))
        return result

    forwards = []

    def pass_on(slot, view, send, recv):
        for here, copy in passed(slot, view, send, recv):
            pl.when(here)(copy.start)
            forwards.append((here, copy))

    middle = sorted({2, n - 2}) + list(range(3, n - 2)) if relayed else []
    order = middle + [step for step in range(1, n) if step not in middle]
    arrivals = [n - step for step in order]
    if relayed:
        near = jnp.where(kv == n - 1, n - 1, 1)
        arrivals = middle + [near, n - near]
    first = {}
    for step in order:
        first[step] = to_chip(
            xg.at[0, tp], xg.at[n - step, tp], step, s1.at[step], r1.at[n - step]
        )
        direct(step, first[step].start)
    first_sib = {0: to_sibling(xg.at[0, tp], s1b.at[0], r1b.at[0])}
    first_sib[0].start()

    eye = (
        lax.broadcasted_iota(jnp.int32, (seqs, seqs), 0)
        == lax.broadcasted_iota(jnp.int32, (seqs, seqs), 1)
    ).astype(F32)

    def turn(value):
        return lax.dot_general(eye, value, NT, precision=HIGH, preferred_element_type=F32)

    parent = turn(pred_ref[...].astype(F32))
    admitted = turn(adm_ref[...].astype(F32))[:, :1]
    current = [jnp.full((seqs, 1), float(j), F32) for j in range(props)]
    above = [parent[:, j : j + 1] for j in range(props)]
    onehot = {}
    depth = [jnp.zeros((seqs, 1), F32) for _ in range(props)]
    lineage = {}
    for lag in range(props):
        for j in range(props):
            for i in range(j + 1):
                onehot[lag, j, i] = (current[j] == float(i)).astype(F32)
                lineage[j, i] = lineage.get((j, i), 0.0) + onehot[lag, j, i]
            if lag > 0:
                depth[j] = depth[j] + (current[j] >= 0.0).astype(F32)
        for j in range(props):
            upward = jnp.full((seqs, 1), -1.0, F32)
            for i in range(j + 1):
                hit = onehot[lag, j, i]
                upward = upward + hit * (above[i] + 1.0)
            current[j] = upward
    depth_is = {
        (j, d): (depth[j] == float(d)).astype(F32) for j in range(props) for d in range(j + 1)
    }
    slots = bsave_ref.shape[0]
    pick = [(admitted == float(a)).astype(F32) for a in range(slots - CONV + 2)]

    def previous(save):
        return [
            sum(pick[a] * save(a + back) for a in range(len(pick)))
            for back in range(CONV - 1)
        ]

    def conv(slabs, prev, tap):
        result = []
        for j in range(props):
            total = tap(CONV - 1) * slabs[j]
            for lag in range(1, CONV):
                value = None
                for i in range(j - lag + 1):
                    term = onehot[lag, j, i] * slabs[i]
                    value = term if value is None else value + term
                for d in range(min(lag, j + 1)):
                    term = depth_is[j, d] * prev[CONV - 1 - lag + d]
                    value = term if value is None else value + term
                total = total + tap(CONV - 1 - lag) * value
            result.append(silu(total))
        return result

    for copy in loads[:6]:
        copy.wait()
    gain[...] = gain_ref[...].astype(F32)
    for h in range(heads):
        inc_rows[2 * h : 2 * h + 2, :] = inc[h].astype(F32)
    dtw[...] = inc_rows[...].astype(BF16)

    def pick_rows(block, carry):
        for k in range(4):
            s = block * 4 + k
            for back in range(CONV - 1):
                at = pl.multiple_of(s * heads, heads)
                xprev[back, pl.ds(at, heads), :hd] = xsave[s, slot_ref[s] + back].astype(F32)
        return carry

    lax.fori_loop(0, seqs // 4, pick_rows, 0)
    squares = jnp.zeros((rows, 1), F32)
    acc_b = jnp.zeros((rows, wb.shape[1]), F32)
    acc_c = jnp.zeros((rows, wc.shape[1]), F32)
    acc_dt = jnp.zeros((rows, 2 * heads), F32)
    for place, slot in enumerate([0] + arrivals):
        if place:
            to_chip(xg.at[0, tp], xg.at[slot, tp], 1, s1.at[0], r1.at[slot]).wait_recv()
            pass_on(slot, lambda k: xg.at[k, tp], p1, lambda k: r1.at[k])
            first_sib[place] = to_sibling(xg.at[slot, tp], s1b.at[slot], r1b.at[slot])
            first_sib[place].start()
        to_sibling(xg.at[slot, other], s1b.at[slot], r1b.at[slot]).wait_recv()
        chip = lax.rem(kv + slot, n)
        base = pl.multiple_of(chip * (2 * feat), 2 * feat)
        tokens = jnp.concatenate([xg[slot, 0], xg[slot, 1]], axis=1).astype(F32)
        squares = squares + jnp.sum(tokens * tokens, axis=1, keepdims=True)
        span_k = pl.ds(base, 2 * feat)
        gain_rows = 2 * feat // lanes
        gains = jnp.concatenate(
            [gain[pl.ds(chip * gain_rows + k, 1), :] for k in range(gain_rows)], axis=1
        )
        scaled = (tokens * gains).astype(BF16)
        px = lax.dot_general(scaled, wx[:, span_k], NT, preferred_element_type=F32)
        pz = lax.dot_general(scaled, wz[:, span_k], NT, preferred_element_type=F32)
        if place == 0:
            acc_x[...] = px
            acc_z[...] = pz
        else:
            acc_x[...] += px
            acc_z[...] += pz
        acc_b = acc_b + jnp.dot(scaled, wb[span_k, :], preferred_element_type=F32)
        acc_c = acc_c + jnp.dot(scaled, wc[span_k, :], preferred_element_type=F32)
        acc_dt = acc_dt + lax.dot_general(
            scaled, dtw[:, span_k], NT, preferred_element_type=F32
        )
    r_in = lax.rsqrt(squares / d_model + 1e-06)

    def slabs_of(value):
        return [value[j * seqs : (j + 1) * seqs] for j in range(props)]

    def rounded(value):
        return value.astype(BF16).astype(F32)

    b_conv = conv(
        slabs_of(rounded(acc_b * r_in)),
        previous(lambda w: bsave_ref[w].astype(F32)),
        lambda k: btap_ref[k],
    )
    c_conv = conv(
        slabs_of(rounded(acc_c * r_in)),
        previous(lambda w: csave_ref[w].astype(F32)),
        lambda k: ctap_ref[k],
    )
    for j in range(props):
        cs[pl.ds(j, seqs, stride=props), :] = c_conv[j]

    mine = (
        lax.broadcasted_iota(jnp.int32, (2 * heads, heads), 0)
        == 2 * lax.broadcasted_iota(jnp.int32, (2 * heads, heads), 1) + tp
    ).astype(F32)
    acc_dt = jnp.dot(acc_dt, mine, precision=HIGH, preferred_element_type=F32)
    raw = acc_dt * r_in + offset_ref[...]
    step_size = slabs_of(jnp.maximum(raw, 0.0) + jnp.log1p(jnp.exp(-jnp.abs(raw))))
    rate = jnp.exp(shrink_ref[...])
    fade = [turn(fade_ref[j]) - rate * step_size[j] for j in range(props)]
    level = [
        sum(lineage[j, i] * fade[i] for i in range(j + 1)) for j in range(props)
    ]
    pairs = [(j, i) for j in range(props) for i in range(j + 1)]
    table = []
    for j, i in pairs:
        score = jnp.sum(c_conv[j] * b_conv[i], axis=1, keepdims=True)
        table.append(
            lineage[j, i] * jnp.exp(jnp.minimum(level[j] - level[i], 0.0)) * score * step_size[i]
            + (bypass_ref[...] if i == j else 0.0)
        )
    table += [jnp.exp(level[j]) for j in range(props)]
    table = jnp.concatenate(table, axis=0)
    table_hi = table.astype(BF16)
    table_lo = (table - table_hi.astype(F32)).astype(BF16)

    for copy in st_loads:
        copy.wait()
    pack = 8 // props
    order2 = order
    second = {}
    second_sib = {}
    for ch in range(chunks):
        cols = slice(ch * cw, (ch + 1) * cw)

        def group(g, carry):
            at = pl.multiple_of(g * 8, 8)
            reads = cs[pl.ds(at, 8), :].astype(BF16)
            row = lax.broadcasted_iota(jnp.int32, (8, cw), 0)
            total = None
            for k in range(pack):
                state = st[g * pack + k, ch * cw : (ch + 1) * cw, :].astype(BF16)
                part = lax.dot_general(reads, state, NT, preferred_element_type=F32)
                total = part if total is None else jnp.where(row < k * props, total, part)
            for lane in range(cw // lanes):
                ys[lane, pl.ds(at, 8), :] = total[:, lane * lanes : (lane + 1) * lanes]
            return carry

        def block(q, carry):
            for k in range(4):
                group(q * 4 + k, 0)
            return carry

        lax.fori_loop(0, seqs // pack // 4, block, 0)

        spread = (
            lax.broadcasted_iota(jnp.int32, (heads, cw), 0)
            == (lax.broadcasted_iota(jnp.int32, (heads, cw), 1) + ch * cw) // hd
        ).astype(BF16)
        mix = jnp.dot(table_hi, spread, preferred_element_type=F32) + jnp.dot(
            table_lo, spread, preferred_element_type=F32
        )
        x_conv = conv(
            slabs_of(rounded(acc_x[:, cols] * r_in)),
            [
                jnp.concatenate(
                    [
                        xprev[back, pl.ds(ch * hpc + h, seqs, stride=heads), :][:, :hd]
                        for h in range(hpc)
                    ],
                    axis=1,
                )
                for back in range(CONV - 1)
            ],
            lambda k: jnp.concatenate(
                [xtap_ref[k, ch * hpc + h] for h in range(hpc)], axis=1
            ),
        )
        gate = slabs_of(silu(rounded(acc_z[:, cols] * r_in)))
        for j in range(props):
            carried = jnp.concatenate(
                [ys[lane, pl.ds(j, seqs, stride=props), :] for lane in range(cw // lanes)], axis=1
            )
            at = (len(pairs) + j) * seqs
            y = mix[at : at + seqs] * carried
            for index, (to, i) in enumerate(pairs):
                if to == j:
                    y = y + mix[index * seqs : (index + 1) * seqs] * x_conv[i]
            gg[0, tp, ch, pl.ds(j * seqs, seqs), :] = (y * gate[j]).astype(BF16)
        for step in order2:
            second[step, ch] = to_chip(
                gg.at[0, tp, ch], gg.at[n - step, tp, ch], step,
                s2.at[step, ch], r2.at[n - step, ch],
            )
            direct(step, second[step, ch].start)
        second_sib[0, ch] = to_sibling(gg.at[0, tp, ch], s2b.at[0, ch], r2b.at[0, ch])
        second_sib[0, ch].start()

    loads[6].wait()
    product = jnp.zeros((rows, fl.shape[3]), F32)
    total_sq = jnp.zeros((rows, 1), F32)

    def add_piece(product, total_sq, slot, core, ch):
        value = gg[slot, core, ch]
        chip = lax.rem(kv + slot, n)
        weight = fl[pl.ds(chip * heads + ch * hpc, hpc), core].reshape(cw, fl.shape[3])
        product = product + jnp.dot(value, weight, preferred_element_type=F32)
        value = value.astype(F32)
        return product, total_sq + jnp.sum(value * value, axis=1, keepdims=True)

    for ch in range(chunks):
        product, total_sq = add_piece(product, total_sq, 0, tp, ch)
    for ch in range(chunks):
        to_sibling(gg.at[0, other, ch], s2b.at[0, ch], r2b.at[0, ch]).wait_recv()
        product, total_sq = add_piece(product, total_sq, 0, other, ch)
    for place, (slot, ch) in enumerate((slot, ch) for slot in arrivals for ch in range(chunks)):
        to_chip(
            gg.at[0, tp, ch], gg.at[slot, tp, ch], 1, s2.at[0, ch], r2.at[slot, ch]
        ).wait_recv()
        pass_on(slot, lambda k, ch=ch: gg.at[k, tp, ch], p2.at[ch], lambda k, ch=ch: r2.at[k, ch])
        second_sib[place + 1, ch] = to_sibling(
            gg.at[slot, tp, ch], s2b.at[slot, ch], r2b.at[slot, ch]
        )
        second_sib[place + 1, ch].start()
        product, total_sq = add_piece(product, total_sq, slot, tp, ch)
        to_sibling(gg.at[slot, other, ch], s2b.at[slot, ch], r2b.at[slot, ch]).wait_recv()
        product, total_sq = add_piece(product, total_sq, slot, other, ch)
    r_out = lax.rsqrt(total_sq / (heads_all * hd) + 1e-05)
    out_ref[...] = (product * r_out).astype(BF16)
    for step, copy in first.items():
        direct(step, copy.wait_send)
    for (step, _), copy in second.items():
        direct(step, copy.wait_send)
    for copy in list(first_sib.values()) + list(second_sib.values()):
        copy.wait_send()
    for here, copy in forwards:
        pl.when(here)(copy.wait_send)


def shards(
    candidate_vectors,
    leading_scaling_factor,
    lane_feed_matrix,
    final_valve_matrix,
    increment_matrix,
    entry_basis_matrix,
    readout_basis_matrix,
    lane_feed_kernel,
    entry_basis_kernel,
    readout_basis_kernel,
    increment_offset,
    shrink_speed_exponent,
    lane_bypass_factor,
    final_linear_matrix,
    hidden_carried_memory,
    lane_filter_memory,
    entry_basis_memory,
    readout_basis_memory,
    predecessor_index,
    admitted_counts,
    surplus_fading,
):
    seqs, props, feat = candidate_vectors.shape
    heads = increment_offset.shape[0]
    hd = lane_feed_matrix.shape[3]
    d_model = lane_feed_matrix.shape[0]
    state = hidden_carried_memory.shape[4]
    window = lane_filter_memory.shape[1]
    heads_all, groups, _, out_cols = final_linear_matrix.shape
    n = lax.axis_size("kv")
    rows = seqs * props
    wide = heads * hd
    chunks = max(1, wide // 256)
    cw = wide // chunks
    wx = lane_feed_matrix.transpose(1, 2, 3, 0).reshape(wide, d_model)
    wz = final_valve_matrix.transpose(1, 2, 3, 0).reshape(wide, d_model)
    wb = entry_basis_matrix.reshape(d_model, state)
    wc = readout_basis_matrix.reshape(d_model, state)
    args = (
        candidate_vectors,
        leading_scaling_factor.reshape(d_model // 128, 128),
        wx,
        wz,
        increment_matrix.transpose(1, 2, 0),
        wb,
        wc,
        lane_feed_kernel,
        entry_basis_kernel,
        readout_basis_kernel,
        increment_offset.reshape(1, heads),
        shrink_speed_exponent.reshape(1, heads),
        lane_bypass_factor.reshape(1, heads),
        final_linear_matrix,
        hidden_carried_memory.reshape(seqs, wide, state),
        lane_filter_memory.reshape(seqs, window, heads, hd),
        entry_basis_memory.transpose(1, 2, 0, 3).reshape(window, seqs, state),
        readout_basis_memory.transpose(1, 2, 0, 3).reshape(window, seqs, state),
        predecessor_index.T,
        admitted_counts.reshape(1, seqs),
        admitted_counts,
        surplus_fading.transpose(1, 2, 3, 0).reshape(props, heads, seqs),
    )
    in_hbm = {0, 2, 3, 4, 5, 6, 13, 14, 15}
    in_smem = 20
    vmem = pl.BlockSpec(memory_space=pltpu.VMEM)
    anywhere = pl.BlockSpec(memory_space=pl.ANY)
    scalars = pl.BlockSpec(memory_space=pltpu.SMEM)
    dma = pltpu.SemaphoreType.DMA
    tiles = max(1, feat // 128)
    mixed = pl.pallas_call(
        functools.partial(
            mixer_kernel, n, seqs, props, heads, hd, chunks, d_model, heads_all * groups
        ),
        out_shape=jax.ShapeDtypeStruct((rows, out_cols), BF16),
        in_specs=[
            anywhere if k in in_hbm else scalars if k == in_smem else vmem
            for k in range(len(args))
        ],
        out_specs=vmem,
        scratch_shapes=[
            pltpu.VMEM((n, 2, rows, feat), BF16),
            pltpu.VMEM((n, 2, chunks, rows, cw), BF16),
            pltpu.VMEM((wide, d_model), BF16),
            pltpu.VMEM((wide, d_model), BF16),
            pltpu.VMEM((d_model, state), BF16),
            pltpu.VMEM((d_model, state), BF16),
            pltpu.VMEM(final_linear_matrix.shape, BF16),
            pltpu.VMEM((seqs, wide, state), F32),
            pltpu.VMEM((rows, wide), F32),
            pltpu.VMEM((rows, wide), F32),
            pltpu.VMEM((rows, state), F32),
            pltpu.VMEM((cw // 128, rows, 128), F32),
            pltpu.VMEM((seqs, props, feat), BF16),
            pltpu.VMEM((tiles, rows, 128), F32),
            pltpu.VMEM((d_model // 128, 128), F32),
            pltpu.VMEM((heads, groups, d_model), BF16),
            pltpu.VMEM((heads * groups, d_model), F32),
            pltpu.VMEM((heads * groups, d_model), BF16),
            pltpu.VMEM((seqs, window, heads, hd), BF16),
            pltpu.VMEM((CONV - 1, seqs * heads, 128), F32),
            dma((7,)),
            dma((4,)),
            dma,
            dma((n,)),
            dma((n,)),
            dma((n,)),
            dma((n,)),
            dma((n, chunks)),
            dma((n, chunks)),
            dma((n, chunks)),
            dma((n, chunks)),
            dma,
            dma((chunks,)),
        ],
        compiler_params=pltpu.CompilerParams(collective_id=0, has_side_effects=True),
    )(*args)
    return mixed.reshape(props, seqs, out_cols).transpose(1, 0, 2)


def solution(mesh):
    placed = (
        P(("grp", "dp"), None, ("kv", "tp")),
        P(),
        P(None, "kv", "tp", None),
        P(None, "kv", "tp", None),
        P(),
        P(None, "tp", None),
        P(None, "tp", None),
        P(None, "kv", "tp", None),
        P(None, "tp", None),
        P(None, "tp", None),
        P("kv", "tp"),
        P("kv", "tp"),
        P("kv", "tp"),
        P(None, None, None, ("kv", "tp")),
        P(("grp", "dp"), "kv", "tp", None, None),
        P(("grp", "dp"), None, "kv", "tp", None),
        P(("grp", "dp"), None, "tp", None),
        P(("grp", "dp"), None, "tp", None),
        P(("grp", "dp"), None),
        P(("grp", "dp")),
        P(("grp", "dp"), None, "kv", "tp"),
    )
    return jax.shard_map(
        shards,
        mesh=mesh,
        in_specs=placed,
        out_specs=P(("grp", "dp"), None, ("kv", "tp")),
        check_vma=False,
    )
```
